32 devices in a mesh: sp: 8 (over z, y), tp: 4 (over x, core).
Axes of the slice: x: 2, y: 2, z: 4, core: 2. Of those that a mesh axis runs over, the one named last changes fastest.
Arguments:
- stream: bfloat16 [4096, 2048], P(('sp', 'tp')), may hold values from -6 to 6
- query_rows: bfloat16 [4096, 1024], P('sp', 'tp'), may hold values from -6 to 6
- key_rows: bfloat16 [4096, 1024], P('sp', 'tp'), may hold values from -6 to 6
- value_rows: bfloat16 [4096, 1024], P('sp', 'tp'), may hold values from -6 to 6
- log_decay: float32 [4096, 1024], P('sp', 'tp'), may hold values from -0.8 to 0, as said below
- head_gain: float32 [1024], P('tp'), may hold values from 0.1 to 1.9
- out_weight: bfloat16 [1024, 2048], replicated, may hold values from -0.1875 to 0.1875
- ffn_gain: float32 [2048], replicated, may hold values from 0.1 to 1.9
- expert_ids: int32 [4096, 2], P(('sp', 'tp')), may hold values from 0 to 31, as said below
- group_prob: float32 [4096], P(('sp', 'tp')), may hold values from 0.3 to 1
- pick_logits: float32 [4096, 2], P(('sp', 'tp')), may hold values from -6 to 6
- gate_weight: bfloat16 [32, 2048, 1024], P(('sp', 'tp')), may hold values from -0.125 to 0.125
- up_weight: bfloat16 [32, 2048, 1024], P(('sp', 'tp')), may hold values from -0.125 to 0.125
- down_weight: bfloat16 [32, 1024, 2048], P(('sp', 'tp')), may hold values from -0.1875 to 0.1875
Outputs:
- layer_out: bfloat16 [4096, 2048], P(('sp', 'tp'))
The draws below stay inside these ranges and needn't reach their ends.
Inputs may be any that keep to these rules, and one draw needn't show every extreme that they name: `log_decay`: entries are negative. `expert_ids`: A token's two experts are different and lie in one group of 8 consecutive expert numbers. Among the 128 tokens of one device (aligned blocks of 128 tokens) no expert is named more than 16 times; in every draw the experts of one group are each named exactly 16 times by the tokens of every device.
All inputs are finite; a program needn't handle non-finite values.
Results may differ from the reference program's by a relative error of at most 0.014.
Values may be sent and summed in bfloat16 or wider, within the bound.
A program may use at most 128 MiB of HBM per device.

```python
import math
import jax
import jax.numpy as jnp
from jax import lax

D = 2048
MIXER_COUNT = 8
KEY_FEATURE_DIM = 128
FF = 1024
GROUPS = 4
TOPK = 2
BLOCK = 64
TOK_DEV = 512
TOKENS = 4096
HK = 1024
EXPERTS = 32
CAP = 16
N_SP = 8
N_TP = 4


def draw_log_decay(key, part):
    base_key = jax.random.fold_in(key, 29)
    keys_all = jax.random.split(base_key, 7)
    context_span = TOK_DEV * N_SP
    fast_head = jax.random.randint(keys_all[0], (MIXER_COUNT,), 0, 2) == 1
    slow_rate = jnp.exp(jax.random.uniform(keys_all[1], (MIXER_COUNT, KEY_FEATURE_DIM), jnp.float32, jnp.log(0.1), jnp.log(0.6))) / context_span
    fast_rate = jnp.exp(jax.random.uniform(keys_all[2], (MIXER_COUNT, KEY_FEATURE_DIM), jnp.float32, jnp.log(0.01), jnp.log(1.0 / 30.0)))
    base_rate = jnp.where(fast_head[:, None], fast_rate, slow_rate)
    device_factor = jnp.exp(jax.random.uniform(keys_all[3], (N_SP,), jnp.float32, jnp.log(0.5), jnp.log(2.0)))
    device_factor = jnp.repeat(device_factor, TOK_DEV)
    noise = jnp.exp(0.5 * jnp.clip(jax.random.normal(keys_all[4], (context_span, MIXER_COUNT, KEY_FEATURE_DIM), jnp.float32), -2.5, 2.5))
    spots = jax.random.permutation(keys_all[5], context_span)[:3]
    surviving_proportion = jax.random.uniform(keys_all[6], (3,), jnp.float32, 0.6, 0.8)
    specialist_tallies = jnp.arange(context_span, dtype=jnp.int32)[:, None] == spots[None, :]
    segment_span = jnp.sum(jnp.where(specialist_tallies, jnp.log(surviving_proportion)[None, :], 0.0), axis=1)
    forgetting_factors = base_rate[None] * device_factor[:, None, None] * noise
    return (segment_span[:, None, None] - forgetting_factors).reshape(context_span, MIXER_COUNT * KEY_FEATURE_DIM).astype(jnp.float32)


def group_order(order_key):
    return jax.random.permutation(order_key, EXPERTS // GROUPS)


def draw_expert_ids(key, part):
    base_key = jax.random.fold_in(key, 71)
    big_group = jax.random.randint(jax.random.fold_in(base_key, 1), (), 0, GROUPS)
    per_group = EXPERTS // GROUPS
    block_rows = TOK_DEV // N_TP
    block_count = TOKENS // block_rows

    def one_block(block_key):
        keys_here = jax.random.split(block_key, 4)
        shifted = jax.random.randint(keys_here[0], (block_rows,), 1, GROUPS)
        labels = jnp.where(jnp.arange(block_rows) < block_rows // 2, big_group, (big_group + shifted) % GROUPS)
        labels = jax.random.permutation(keys_here[1], labels)
        onehot = (labels[:, None] == jnp.arange(GROUPS)[None, :]).astype(jnp.int32)
        order_in = jnp.sum(jnp.cumsum(onehot, axis=0) * onehot, axis=1) - 1
        orders = jax.vmap(group_order)(jax.random.split(keys_here[2], GROUPS))
        offsets = jax.random.randint(keys_here[3], (GROUPS,), 1, per_group)
        first = orders[labels, order_in % per_group]
        second = orders[labels, (order_in + offsets[labels]) % per_group]
        return jnp.stack([labels * per_group + first, labels * per_group + second], axis=1)

    def block_key_of(block_number):
        return jax.random.fold_in(base_key, block_number + 2)
    block_keys = jax.vmap(block_key_of)(jnp.arange(block_count))
    return jax.vmap(one_block)(block_keys).reshape(TOKENS, TOPK).astype(jnp.int32)


def block_levels(stream_key, shape, pieces, smallest, top_value):
    def one(position, parts):
        steps = jax.random.uniform(jax.random.fold_in(jax.random.fold_in(stream_key, 6), position), (parts,), jnp.float32, smallest / len(pieces), top_value / len(pieces))
        return jnp.repeat(jnp.exp(steps), shape[position] // parts).reshape((-1,) + (1,) * (len(shape) - position - 1))

    level = one(*pieces[0])
    for cut in pieces[1:]:
        level = level * one(*cut)
    return level


def bell_draw(rng, dims, scale, bound, pieces=(), kind=jnp.bfloat16):
    gain = block_levels(rng, dims, pieces, -0.22, 0.18) if pieces else 1.0
    result = jax.random.normal(rng, dims, jnp.float32) * scale * gain
    return jnp.minimum(jnp.maximum(result, -bound), bound).astype(kind)


def setup_inputs(seed: int = 0) -> dict:
    splits = jax.random.split(jax.random.key(seed), 15)
    return {
        "stream": bell_draw(splits[0], (TOKENS, D), 1.0, 6.0, ((0, 32),)),
        "query_rows": bell_draw(splits[1], (TOKENS, HK), 1.0, 6.0, ((0, 8), (1, 4))),
        "key_rows": bell_draw(splits[2], (TOKENS, HK), 1.0, 6.0, ((0, 8), (1, 4))),
        "value_rows": bell_draw(splits[3], (TOKENS, HK), 1.0, 6.0, ((0, 8), (1, 4))),
        "log_decay": draw_log_decay(jax.random.fold_in(splits[14], 71), 0),
        "head_gain": jnp.clip(1.0 + 0.18 * jax.random.normal(splits[5], (HK,), jnp.float32), 0.1, 1.9),
        "out_weight": bell_draw(splits[6], (HK, D), HK ** -0.5, 0.1875),
        "ffn_gain": jnp.clip(1.0 + 0.18 * jax.random.normal(splits[7], (D,), jnp.float32), 0.1, 1.9),
        "expert_ids": draw_expert_ids(jax.random.fold_in(splits[14], 71), 0),
        "group_prob": jnp.clip(jnp.exp(math.log(1.0) - 1.2039728 * jax.random.uniform(splits[9], (TOKENS,), jnp.float32) ** block_levels(splits[9], (TOKENS,), ((0, 32),), -0.2, 0.2)), 0.3, 1.0),
        "pick_logits": bell_draw(splits[10], (TOKENS, TOPK), 1.5, 6.0, ((0, 32),), jnp.float32),
        "gate_weight": bell_draw(splits[11], (EXPERTS, D, FF), D ** -0.5, 0.125, ((0, 32),)),
        "up_weight": bell_draw(splits[12], (EXPERTS, D, FF), D ** -0.5, 0.125, ((0, 32),)),
        "down_weight": bell_draw(splits[13], (EXPERTS, FF, D), FF ** -0.5, 0.1875, ((0, 32),)),
    }


PRECISE = lax.Precision.HIGHEST
EPSILON = 1e-06

def gla_block(carry_state, step_input):
    query_in, key_in, value_in, decay_log = step_input
    query_all = query_in.astype(jnp.float32) * KEY_FEATURE_DIM ** (-0.5)
    key_all = key_in.astype(jnp.float32)
    value_all = value_in.astype(jnp.float32)
    cumulative = jnp.cumsum(decay_log, axis=0)
    q_dec = query_all * jnp.exp(cumulative)
    k_dec = key_all * jnp.exp(-cumulative)
    scores = jnp.einsum('ihd,jhd->hij', q_dec, k_dec, precision=PRECISE)
    positions = jnp.arange(query_all.shape[0], dtype=jnp.int32)
    causal = positions[:, None] >= positions[None, :]
    scores = jnp.where(causal[None], scores, jnp.float32(0.0))
    in_block = jnp.einsum('hij,jhe->ihe', scores, value_all, precision=PRECISE)
    carried = jnp.einsum('ihd,hde->ihe', q_dec, carry_state, precision=PRECISE)
    block_fall = cumulative[-1]
    key_last = key_all * jnp.exp(block_fall[None] - cumulative)
    update = jnp.einsum('jhd,jhe->hde', key_last, value_all, precision=PRECISE)
    carry_state = carry_state * jnp.exp(block_fall)[:, :, None] + update
    return (carry_state, in_block + carried)

def reference(stream, query_rows, key_rows, value_rows, log_decay, head_gain, out_weight, ffn_gain, expert_ids, group_prob, pick_logits, gate_weight, up_weight, down_weight):
    block_count = TOKENS // BLOCK

    def as_blocks(array):
        return array.reshape(block_count, BLOCK, MIXER_COUNT, KEY_FEATURE_DIM)
    start_state = jnp.zeros((MIXER_COUNT, KEY_FEATURE_DIM, KEY_FEATURE_DIM), jnp.float32)
    _, heads_out = lax.scan(gla_block, start_state, (as_blocks(query_rows), as_blocks(key_rows), as_blocks(value_rows), as_blocks(log_decay)))
    heads_out = heads_out.reshape(TOKENS, MIXER_COUNT, KEY_FEATURE_DIM)
    mean_sq = lax.optimization_barrier(jnp.mean(heads_out * heads_out, axis=-1, keepdims=True))
    attn_rows = (heads_out * lax.rsqrt(mean_sq + EPSILON) * head_gain.reshape(MIXER_COUNT, KEY_FEATURE_DIM)).reshape(TOKENS, HK)
    attn_rows = attn_rows.astype(jnp.bfloat16)
    projected = jnp.dot(attn_rows, out_weight, preferred_element_type=jnp.float32)
    mixed_rows = (stream.astype(jnp.float32) + projected).astype(jnp.bfloat16)
    mixed32 = mixed_rows.astype(jnp.float32)
    normed = mixed32 * lax.rsqrt(lax.optimization_barrier(jnp.mean(mixed32 * mixed32, axis=-1, keepdims=True)) + EPSILON) * ffn_gain
    normed = normed.astype(jnp.bfloat16)
    devices = N_SP * N_TP
    row_count = TOKENS // devices
    flat_ids = expert_ids.reshape(devices, row_count * TOPK)
    onehot = (flat_ids[:, :, None] == jnp.arange(EXPERTS, dtype=jnp.int32)[None, None, :]).astype(jnp.int32)
    slot_rank = lax.optimization_barrier(jnp.sum(jnp.cumsum(onehot, axis=1) * onehot, axis=2)) - 1
    dev_index = jnp.broadcast_to(jnp.arange(devices, dtype=jnp.int32)[:, None], flat_ids.shape)
    token_index = dev_index * row_count + jnp.arange(row_count * TOPK, dtype=jnp.int32)[None, :] // TOPK
    slot_table = jnp.full((EXPERTS, devices, CAP), TOKENS, jnp.int32)
    slot_table = slot_table.at[flat_ids, dev_index, slot_rank].set(token_index)
    padded = jnp.concatenate([normed, jnp.zeros((1, D), jnp.bfloat16)], axis=0)

    def one_expert(inputs):
        expert_index, gate_mat, up_mat, down_mat = inputs
        rows_in = padded[expert_index.reshape(-1)]
        gate_act = jnp.dot(rows_in, gate_mat, preferred_element_type=jnp.float32)
        up_act = jnp.dot(rows_in, up_mat, preferred_element_type=jnp.float32)
        hidden = (jax.nn.silu(gate_act) * up_act).astype(jnp.bfloat16)
        return jnp.dot(hidden, down_mat, preferred_element_type=jnp.float32).astype(jnp.bfloat16)
    outputs = lax.map(one_expert, (slot_table, gate_weight, up_weight, down_weight))
    outputs = outputs.reshape(EXPERTS, devices, CAP, D)
    picked = outputs[flat_ids, dev_index, slot_rank].reshape(TOKENS, TOPK, D)
    logit_gap = pick_logits[:, 0] - pick_logits[:, 1]
    first_weight = group_prob * jax.nn.sigmoid(logit_gap)
    second_weight = group_prob * jax.nn.sigmoid(-logit_gap)
    branch = first_weight[:, None] * picked[:, 0].astype(jnp.float32) + second_weight[:, None] * picked[:, 1].astype(jnp.float32)
    return (mixed32 + branch).astype(jnp.bfloat16)
```

```python
import functools

import jax
import jax.numpy as jnp
from jax import lax
from jax.experimental import pallas as pl
from jax.experimental.pallas import tpu as pltpu
from jax.sharding import PartitionSpec as P

KEY_FEATURE_DIM = 128
TOPK = 2
BLOCK = 64
GROUPS = 4
EPSILON = 1e-06
F32 = jnp.float32
BF16 = jnp.bfloat16
MESH = pl.DeviceIdType.MESH
VMEM_LIMIT = 60 * 1024 * 1024


def dot(a, b):
    return jnp.dot(a, b, preferred_element_type=F32)


def dot_nt(a, b):
    return lax.dot_general(a, b, (((1,), (1,)), ((), ())), preferred_element_type=F32)


def dot_tn(a, b):
    return lax.dot_general(a, b, (((0,), (0,)), ((), ())), preferred_element_type=F32)


def iota(shape, axis):
    return lax.broadcasted_iota(jnp.int32, shape, axis)


def mixer_kernel(
    n_sp, n_tp, capp,
    q_ref, k_ref, v_ref, decay_ref, gain_ref, stream_ref, ow_hbm, ffn_ref, ids_ref, prob_ref,
    logit_ref,
    mixed_ref, rows_ref, wc_ref, gsel_ref,
    qd, kd, rw, st_in, within, ow, inc_s, inc_f, exc_s, exc_f,
    s_send, s_recv, f_send, f_recv, attn, arecv,
    ow_sem, ss_sem, sr_sem, fs_sem, fr_sem, as_sem, ar_sem,
):
    me, tp = lax.axis_index("sp"), lax.axis_index("tp")
    tokens, cols = q_ref.shape
    heads = cols // KEY_FEATURE_DIM
    blocks = tokens // BLOCK
    row_count = stream_ref.shape[0]
    model = stream_ref.shape[1]
    steps = s_send.shape[0]

    barrier = pltpu.get_barrier_semaphore()
    for i in range(1, n_sp):
        pl.semaphore_signal(
            barrier, inc=1, device_id=(lax.rem(me + i, n_sp), tp), device_id_type=MESH)
    for i in range(1, n_tp):
        pl.semaphore_signal(
            barrier, inc=1, device_id=(me, lax.rem(tp + i, n_tp)), device_id_type=MESH)
    ow_copy = pltpu.make_async_copy(ow_hbm, ow, ow_sem)
    ow_copy.start()

    tri = (iota((BLOCK, BLOCK), 0) >= iota((BLOCK, BLOCK), 1)).astype(F32)
    tri16 = tri.astype(BF16)
    scale = KEY_FEATURE_DIM ** (-0.5)
    state = [jnp.zeros((KEY_FEATURE_DIM, KEY_FEATURE_DIM), F32) for _ in range(heads)]
    start = jnp.zeros((1, cols), F32)
    for n in range(blocks):
        rows = slice(n * BLOCK, (n + 1) * BLOCK)
        g = decay_ref[rows, :]
        hi = g.astype(BF16)
        rest = g - hi.astype(F32)
        mid = rest.astype(BF16)
        low = (rest - mid.astype(F32)).astype(BF16)
        cum = dot(tri16, hi) + dot(tri16, mid) + dot(tri16, low)
        fall = cum[BLOCK - 1 : BLOCK, :]
        kf = k_ref[rows, :].astype(F32)
        q_dec = q_ref[rows, :].astype(F32) * scale * jnp.exp(cum)
        qd[rows, :] = q_dec.astype(BF16)
        rw[rows, :] = (q_dec * jnp.exp(start)).astype(BF16)
        kd[rows, :] = (kf * jnp.exp(-cum)).astype(BF16)
        k_last = (kf * jnp.exp(fall - cum)).astype(BF16)
        keep = jnp.exp(fall)
        for h in range(heads):
            ch = slice(h * KEY_FEATURE_DIM, (h + 1) * KEY_FEATURE_DIM)
            st_in[n, h] = state[h].astype(BF16)
            state[h] = state[h] * keep[:, ch] + dot_tn(v_ref[rows, ch], k_last[:, ch])
        start = start + fall
    for h in range(heads):
        inc_s[h] = state[h]
        exc_s[h] = jnp.zeros_like(state[h])
    inc_f[...] = jnp.broadcast_to(jnp.exp(start), inc_f.shape)
    exc_f[...] = jnp.ones_like(exc_f)

    pl.semaphore_wait(barrier, n_sp - 1 + n_tp - 1)

    def state_copies(s):
        to = (lax.rem(me + 2 ** s, n_sp), tp)
        return (
            pltpu.make_async_remote_copy(
                s_send.at[s], s_recv.at[s], ss_sem.at[s], sr_sem.at[s],
                device_id=to, device_id_type=MESH),
            pltpu.make_async_remote_copy(
                f_send.at[s], f_recv.at[s], fs_sem.at[s], fr_sem.at[s],
                device_id=to, device_id_type=MESH),
        )

    def send_state(s):
        s_send[s] = inc_s[...].astype(BF16)
        f_send[s] = inc_f[...]

        @pl.when(me + 2 ** s < n_sp)
        def _():
            for copy in state_copies(s):
                copy.start()

    send_state(0)

    experts = n_sp * n_tp
    per_group = experts // GROUPS
    group_cap = rows_ref.shape[0] // GROUPS
    slots = per_group * capp
    ids = ids_ref[...]
    id0, id1 = ids[:, 0:1], ids[:, 1:2]
    oh0 = (iota((row_count, experts), 1) == id0).astype(F32)
    oh1 = (iota((row_count, experts), 1) == id1).astype(F32)
    before = (iota((row_count, row_count), 0) > iota((row_count, row_count), 1)).astype(BF16)
    counts = dot(before, (oh0 + oh1).astype(BF16))
    rank0 = jnp.sum(counts * oh0, axis=1, keepdims=True).astype(jnp.int32)
    rank1 = jnp.sum(counts * oh1, axis=1, keepdims=True).astype(jnp.int32)
    group = id0 // per_group
    ohg = (iota((row_count, KEY_FEATURE_DIM), 1) == group).astype(F32)
    rank_g = jnp.sum(dot(before, ohg.astype(BF16)) * ohg, axis=1, keepdims=True).astype(jnp.int32)
    place = group * group_cap + rank_g
    gsel = (iota((row_count, GROUPS * group_cap), 1) == place).astype(F32).astype(BF16)
    gsel_ref[...] = gsel
    slot0 = (id0 - group * per_group) * capp + rank0
    slot1 = (id1 - group * per_group) * capp + rank1
    logits = logit_ref[...]
    gap = logits[:, 0:1] - logits[:, 1:2]
    w0 = prob_ref[...] / (1.0 + jnp.exp(-gap))
    w1 = prob_ref[...] / (1.0 + jnp.exp(gap))
    slot_iota = iota((row_count, slots), 1)
    w_tok = jnp.where(slot_iota == slot0, w0, 0.0) + jnp.where(slot_iota == slot1, w1, 0.0)
    wc_ref[...] = dot_tn(gsel, w_tok.astype(BF16)).astype(BF16)

    for n in range(blocks):
        rows = slice(n * BLOCK, (n + 1) * BLOCK)
        for h in range(heads):
            ch = slice(h * KEY_FEATURE_DIM, (h + 1) * KEY_FEATURE_DIM)
            scores = jnp.where(tri > 0, dot_nt(qd[rows, ch], kd[rows, ch]), 0.0)
            within[rows, ch] = dot(scores.astype(BF16), v_ref[rows, ch]) + dot_nt(
                qd[rows, ch], st_in[n, h])

    for s in range(steps):
        if s > 0:
            send_state(s)

        @pl.when(me >= 2 ** s)
        def _(s=s):
            for copy in state_copies(s):
                copy.wait_recv()
            for h in range(heads):
                ch = slice(h * KEY_FEATURE_DIM, (h + 1) * KEY_FEATURE_DIM)
                got = s_recv[s, h].astype(F32)
                exc_s[h] = got * exc_f[0:1, ch] + exc_s[h]
                inc_s[h] = got * inc_f[0:1, ch] + inc_s[h]
            exc_f[...] = exc_f[...] * f_recv[s]
            inc_f[...] = inc_f[...] * f_recv[s]

    for h in range(heads):
        ch = slice(h * KEY_FEATURE_DIM, (h + 1) * KEY_FEATURE_DIM)
        out = within[:, ch] + dot_nt(rw[:, ch], exc_s[h].astype(BF16))
        mean_sq = jnp.mean(out * out, axis=-1, keepdims=True)
        out = (out * lax.rsqrt(mean_sq + EPSILON) * gain_ref[:, ch]).astype(BF16)
        for t in range(n_tp):
            attn[t, :, ch] = out[t * row_count : (t + 1) * row_count]

    def attn_copy(i):
        to = lax.rem(tp + i, n_tp)
        return pltpu.make_async_remote_copy(
            attn.at[to], arecv.at[tp], as_sem.at[i], ar_sem.at[i],
            device_id=(me, to), device_id_type=MESH)

    for i in range(1, n_tp):
        attn_copy(i).start()
    arecv[tp] = attn[tp]
    for s in range(steps):
        @pl.when(me + 2 ** s < n_sp)
        def _(s=s):
            for copy in state_copies(s):
                copy.wait_send()
    ow_copy.wait()
    for i in range(1, n_tp):
        attn_copy(i).wait_recv()
    x = jnp.concatenate([arecv[t] for t in range(n_tp)], axis=1)
    tile = 512
    total = jnp.zeros((row_count, 1), F32)
    for c in range(0, model, tile):
        cs = slice(c, c + tile)
        mixed = (stream_ref[:, cs].astype(F32) + dot(x, ow[:, cs])).astype(BF16)
        mixed_ref[:, cs] = mixed
        mixed32 = mixed.astype(F32)
        total = total + jnp.sum(mixed32 * mixed32, axis=1, keepdims=True)
    inv = lax.rsqrt(total / model + EPSILON)
    for c in range(0, model, tile):
        cs = slice(c, c + tile)
        normed = (mixed_ref[:, cs].astype(F32) * inv * ffn_ref[:, cs]).astype(BF16)
        rows_ref[:, cs] = dot_tn(gsel, normed).astype(BF16)
    for i in range(1, n_tp):
        attn_copy(i).wait_send()


def experts_kernel(
    n_tp, per_group,
    rows_ref, wc_ref, gsel_ref, mixed_ref, gate_hbm, up_hbm, down_hbm,
    out_ref,
    gate, up, down, zrow, zw, stage, xbuf, hid, ybuf, back, ret, zret,
    w_sem, zs_sem, zr_sem, ws_sem, wr_sem, ps_sem, pr_sem, bs_sem, br_sem, rs_sem, rr_sem,
):
    idx = lax.axis_index("sp") * n_tp + lax.axis_index("tp")
    z, p = idx // per_group, lax.rem(idx, per_group)
    cap = zrow.shape[1]
    capp = stage.shape[2]
    slots = per_group * capp
    model = out_ref.shape[1]
    ff = hid.shape[1]

    def device(plane, place):
        flat = plane * per_group + place
        return (flat // n_tp, lax.rem(flat, n_tp))

    weights = [
        pltpu.make_async_copy(gate_hbm.at[0], gate, w_sem.at[0]),
        pltpu.make_async_copy(up_hbm.at[0], up, w_sem.at[1]),
        pltpu.make_async_copy(down_hbm.at[0], down, w_sem.at[2]),
    ]
    barrier = pltpu.get_barrier_semaphore()
    for i in range(1, GROUPS):
        pl.semaphore_signal(
            barrier, inc=1, device_id=device(lax.rem(z + i, GROUPS), p), device_id_type=MESH)

    @pl.loop(1, per_group)
    def _(i):
        pl.semaphore_signal(
            barrier, inc=1, device_id=device(z, lax.rem(p + i, per_group)), device_id_type=MESH)

    for copy in weights:
        copy.start()
    pl.semaphore_wait(barrier, GROUPS - 1 + per_group - 1)

    def plane_rows(k):
        to = lax.rem(z + k, GROUPS)
        return (
            pltpu.make_async_remote_copy(
                wc_ref.at[pl.ds(pl.multiple_of(to * cap, cap), cap)], zw.at[k],
                ws_sem.at[k], wr_sem.at[k], device_id=device(to, p), device_id_type=MESH),
            pltpu.make_async_remote_copy(
                rows_ref.at[pl.ds(pl.multiple_of(to * cap, cap), cap)], zrow.at[k],
                zs_sem.at[k], zr_sem.at[k], device_id=device(to, p), device_id_type=MESH),
        )

    def plane_return(k):
        to = lax.rem(z + GROUPS - k, GROUPS)
        return pltpu.make_async_remote_copy(
            ret.at[k], zret.at[k], rs_sem.at[k], rr_sem.at[k],
            device_id=device(to, p), device_id_type=MESH)

    def piece(k, i):
        to = lax.rem(p + i, per_group)
        return pltpu.make_async_remote_copy(
            stage.at[k, to], xbuf.at[k, p], ps_sem.at[k, i], pr_sem.at[k, i],
            device_id=device(z, to), device_id_type=MESH)

    def piece_back(k, i):
        to = lax.rem(p + i, per_group)
        return pltpu.make_async_remote_copy(
            ybuf.at[k, to], back.at[k, p], bs_sem.at[k, i], br_sem.at[k, i],
            device_id=device(z, to), device_id_type=MESH)

    for k in range(1, GROUPS):
        for copy in plane_rows(k):
            copy.start()
    own = pl.ds(pl.multiple_of(z * cap, cap), cap)
    zrow[0] = rows_ref[own, :]
    zw[0] = wc_ref[own, :]
    tile = 512

    def dispatch(k):
        if k > 0:
            for copy in plane_rows(k):
                copy.wait_recv()
        sel = (zw[k].astype(F32) > 0).astype(F32).astype(BF16)
        for c in range(0, model, tile):
            cs = slice(c, c + tile)
            stage[k, :, :, cs] = dot_tn(sel, zrow[k, :, cs]).astype(BF16).reshape(
                per_group, capp, tile)

        @pl.loop(1, per_group)
        def _(i):
            piece(k, i).start()

        xbuf[k, p] = stage[k, p]

    def expert(k):
        @pl.loop(1, per_group)
        def _(i):
            piece(k, i).wait_recv()

        x = xbuf.at[k]

        @pl.loop(0, ff // 256)
        def _(f):
            fs = pl.ds(pl.multiple_of(f * 256, 256), 256)
            rows = x[...].reshape(slots, model)
            g = dot(rows, gate[:, fs])
            u = dot(rows, up[:, fs])
            hid[:, fs] = (g / (1.0 + jnp.exp(-g)) * u).astype(BF16)

        @pl.loop(0, model // tile)
        def _(c):
            cs = pl.ds(pl.multiple_of(c * tile, tile), tile)
            ybuf[k, :, :, cs] = dot(hid[...], down[:, cs]).astype(BF16).reshape(
                per_group, capp, tile)

        @pl.loop(1, per_group)
        def _(i):
            piece_back(k, i).start()

        back[k, p] = ybuf[k, p]

    def combine(k):
        @pl.loop(1, per_group)
        def _(i):
            piece_back(k, i).wait_recv()

        w = zw[k]
        for c in range(0, model, tile):
            cs = slice(c, c + tile)
            y = dot(w, back[k, :, :, cs].reshape(slots, tile)).astype(BF16)
            if k == 0:
                zret[0, :, cs] = y
            else:
                ret[k, :, cs] = y
        if k > 0:
            plane_return(k).start()

    dispatch(0)
    for copy in weights:
        copy.wait()
    dispatch(1)
    expert(0)
    dispatch(2)
    expert(1)
    combine(0)
    dispatch(3)
    combine(1)
    expert(2)
    combine(2)
    expert(3)
    combine(3)

    for k in range(1, GROUPS):
        plane_return(k).wait_recv()
    gsel = [
        gsel_ref[:, g * cap : (g + 1) * cap] for g in range(GROUPS)
    ]
    for c in range(0, model, tile):
        cs = slice(c, c + tile)
        acc = mixed_ref[:, cs].astype(F32)
        for g in range(GROUPS):
            acc = acc + dot(gsel[g], zret[lax.rem(g - z + GROUPS, GROUPS), :, cs])
        out_ref[:, cs] = acc.astype(BF16)

    for k in range(1, GROUPS):
        for copy in plane_rows(k):
            copy.wait_send()
        plane_return(k).wait_send()
    for k in range(GROUPS):
        @pl.loop(1, per_group)
        def _(i, k=k):
            piece(k, i).wait_send()
            piece_back(k, i).wait_send()


def local(
    stream, query_rows, key_rows, value_rows, log_decay, head_gain, out_weight, ffn_gain,
    expert_ids, group_prob, pick_logits, gate_weight, up_weight, down_weight,
):
    n_sp, n_tp = lax.axis_size("sp"), lax.axis_size("tp")
    tokens, cols = query_rows.shape
    heads = cols // KEY_FEATURE_DIM
    blocks = tokens // BLOCK
    row_count, model = stream.shape
    devices = n_sp * n_tp
    per_group = devices // GROUPS
    cap = 2 * row_count * TOPK // devices
    capp = -(-cap // 16) * 16
    group_cap = per_group * cap // TOPK
    slots = per_group * capp
    ff = gate_weight.shape[2]
    steps = max(1, (n_sp - 1).bit_length())
    kd = KEY_FEATURE_DIM
    vm = pl.BlockSpec(memory_space=pltpu.VMEM)
    anyspace = pl.BlockSpec(memory_space=pl.ANY)
    dma = pltpu.SemaphoreType.DMA
    mixed, rows, wc, gsel = pl.pallas_call(
        functools.partial(mixer_kernel, n_sp, n_tp, capp),
        out_shape=(
            jax.ShapeDtypeStruct((row_count, model), BF16),
            jax.ShapeDtypeStruct((GROUPS * group_cap, model), BF16),
            jax.ShapeDtypeStruct((GROUPS * group_cap, slots), BF16),
            jax.ShapeDtypeStruct((row_count, GROUPS * group_cap), BF16),
        ),
        in_specs=[vm] * 6 + [anyspace] + [vm] * 4,
        out_specs=(vm,) * 4,
        scratch_shapes=[
            pltpu.VMEM((tokens, cols), BF16),
            pltpu.VMEM((tokens, cols), BF16),
            pltpu.VMEM((tokens, cols), BF16),
            pltpu.VMEM((blocks, heads, kd, kd), BF16),
            pltpu.VMEM((tokens, cols), F32),
            pltpu.VMEM(out_weight.shape, BF16),
            pltpu.VMEM((heads, kd, kd), F32),
            pltpu.VMEM((8, cols), F32),
            pltpu.VMEM((heads, kd, kd), F32),
            pltpu.VMEM((8, cols), F32),
            pltpu.VMEM((steps, heads, kd, kd), BF16),
            pltpu.VMEM((steps, heads, kd, kd), BF16),
            pltpu.VMEM((steps, 8, cols), F32),
            pltpu.VMEM((steps, 8, cols), F32),
            pltpu.VMEM((n_tp, row_count, cols), BF16),
            pltpu.VMEM((n_tp, row_count, cols), BF16),
            dma,
            dma((steps,)), dma((steps,)), dma((steps,)), dma((steps,)),
            dma((n_tp,)), dma((n_tp,)),
        ],
        compiler_params=pltpu.CompilerParams(
            collective_id=0, has_side_effects=True, vmem_limit_bytes=VMEM_LIMIT),
    )(
        query_rows, key_rows, value_rows, log_decay, head_gain[None], stream, out_weight,
        ffn_gain[None], expert_ids, group_prob[:, None], pick_logits,
    )
    return pl.pallas_call(
        functools.partial(experts_kernel, n_tp, per_group),
        out_shape=jax.ShapeDtypeStruct((row_count, model), BF16),
        in_specs=[vm] * 4 + [anyspace] * 3,
        out_specs=vm,
        scratch_shapes=[
            pltpu.VMEM((model, ff), BF16),
            pltpu.VMEM((model, ff), BF16),
            pltpu.VMEM((ff, model), BF16),
            pltpu.VMEM((GROUPS, group_cap, model), BF16),
            pltpu.VMEM((GROUPS, group_cap, slots), BF16),
            pltpu.VMEM((GROUPS, per_group, capp, model), BF16),
            pltpu.VMEM((GROUPS, per_group, capp, model), BF16),
            pltpu.VMEM((slots, ff), BF16),
            pltpu.VMEM((GROUPS, per_group, capp, model), BF16),
            pltpu.VMEM((GROUPS, per_group, capp, model), BF16),
            pltpu.VMEM((GROUPS, group_cap, model), BF16),
            pltpu.VMEM((GROUPS, group_cap, model), BF16),
            dma((3,)),
            dma((GROUPS,)), dma((GROUPS,)), dma((GROUPS,)), dma((GROUPS,)),
            dma((GROUPS, per_group)), dma((GROUPS, per_group)),
            dma((GROUPS, per_group)), dma((GROUPS, per_group)),
            dma((GROUPS,)), dma((GROUPS,)),
        ],
        compiler_params=pltpu.CompilerParams(
            collective_id=1, has_side_effects=True, vmem_limit_bytes=VMEM_LIMIT),
    )(rows, wc, gsel, mixed, gate_weight, up_weight, down_weight)


def solution(mesh):
    in_specs = (
        P(("sp", "tp"), None),
        P("sp", "tp"),
        P("sp", "tp"),
        P("sp", "tp"),
        P("sp", "tp"),
        P("tp"),
        P(),
        P(),
        P(("sp", "tp"), None),
        P(("sp", "tp")),
        P(("sp", "tp"), None),
        P(("sp", "tp"), None, None),
        P(("sp", "tp"), None, None),
        P(("sp", "tp"), None, None),
    )
    out_specs = P(("sp", "tp"), None)
    return jax.shard_map(local, mesh=mesh, in_specs=in_specs, out_specs=out_specs, check_vma=False)
```

```python
import functools

import jax
import jax.numpy as jnp
from jax import lax
from jax.experimental import pallas as pl
from jax.experimental.pallas import tpu as pltpu
from jax.sharding import PartitionSpec as P

KEY_FEATURE_DIM = 128
TOPK = 2
BLOCK = 64
GROUPS = 4
EPSILON = 1e-06
F32 = jnp.float32
BF16 = jnp.bfloat16
MESH = pl.DeviceIdType.MESH
VMEM_LIMIT = 63 * 1024 * 1024
SCHEDULE = "D0 W D1 E0 D2 E1 C0 D3 C1 E2 C2 E3 C3"


def dot(a, b):
    return jnp.dot(a, b, preferred_element_type=F32)


def dot_nt(a, b):
    return lax.dot_general(a, b, (((1,), (1,)), ((), ())), preferred_element_type=F32)


def dot_tn(a, b):
    return lax.dot_general(a, b, (((0,), (0,)), ((), ())), preferred_element_type=F32)


def iota(shape, axis):
    return lax.broadcasted_iota(jnp.int32, shape, axis)


def mixer_part(
    n_sp, n_tp, capp, greet,
    q_ref, k_ref, v_ref, decay_ref, gain_ref, stream_ref, ow_hbm, ffn_ref, ids_ref, prob_ref,
    logit_ref,
    mixed_ref, rows_ref, wc_ref, gsel_ref, weights,
    qd, kd, rw, st_in, within, ow, inc_s, inc_f, exc_s, exc_f,
    s_send, s_recv, f_send, f_recv, attn, arecv,
    ow_sem, ss_sem, sr_sem, fs_sem, fr_sem, as_sem, ar_sem,
):
    me, tp = lax.axis_index("sp"), lax.axis_index("tp")
    tokens, cols = q_ref.shape
    heads = cols // KEY_FEATURE_DIM
    blocks = tokens // BLOCK
    row_count = stream_ref.shape[0]
    model = stream_ref.shape[1]
    steps = s_send.shape[0]

    barrier = pltpu.get_barrier_semaphore()
    for i in range(1, n_sp):
        pl.semaphore_signal(
            barrier, inc=1, device_id=(lax.rem(me + i, n_sp), tp), device_id_type=MESH)
    for i in range(1, n_tp):
        pl.semaphore_signal(
            barrier, inc=1, device_id=(me, lax.rem(tp + i, n_tp)), device_id_type=MESH)
    greet()
    ow_copy = pltpu.make_async_copy(ow_hbm, ow, ow_sem)
    ow_copy.start()
    for copy in weights:
        copy.start()

    tri = (iota((BLOCK, BLOCK), 0) >= iota((BLOCK, BLOCK), 1)).astype(F32)
    tri16 = tri.astype(BF16)
    scale = KEY_FEATURE_DIM ** (-0.5)
    state = [jnp.zeros((KEY_FEATURE_DIM, KEY_FEATURE_DIM), F32) for _ in range(heads)]
    start = jnp.zeros((1, cols), F32)
    for n in range(blocks):
        rows = slice(n * BLOCK, (n + 1) * BLOCK)
        g = decay_ref[rows, :]
        hi = g.astype(BF16)
        rest = g - hi.astype(F32)
        mid = rest.astype(BF16)
        low = (rest - mid.astype(F32)).astype(BF16)
        cum = dot(tri16, hi) + dot(tri16, mid) + dot(tri16, low)
        fall = cum[BLOCK - 1 : BLOCK, :]
        kf = k_ref[rows, :].astype(F32)
        q_dec = q_ref[rows, :].astype(F32) * scale * jnp.exp(cum)
        qd[rows, :] = q_dec.astype(BF16)
        rw[rows, :] = (q_dec * jnp.exp(start)).astype(BF16)
        kd[rows, :] = (kf * jnp.exp(-cum)).astype(BF16)
        k_last = (kf * jnp.exp(fall - cum)).astype(BF16)
        keep = jnp.exp(fall)
        for h in range(heads):
            ch = slice(h * KEY_FEATURE_DIM, (h + 1) * KEY_FEATURE_DIM)
            st_in[n, h] = state[h].astype(BF16)
            state[h] = state[h] * keep[:, ch] + dot_tn(v_ref[rows, ch], k_last[:, ch])
        start = start + fall
    for h in range(heads):
        inc_s[h] = state[h]
        exc_s[h] = jnp.zeros_like(state[h])
    inc_f[...] = jnp.broadcast_to(jnp.exp(start), inc_f.shape)
    exc_f[...] = jnp.ones_like(exc_f)

    pl.semaphore_wait(barrier, n_sp - 1 + n_tp - 1 + GROUPS - 1 + n_sp * n_tp // GROUPS - 1)

    def state_copies(s):
        to = (lax.rem(me + 2 ** s, n_sp), tp)
        return (
            pltpu.make_async_remote_copy(
                s_send.at[s], s_recv.at[s], ss_sem.at[s], sr_sem.at[s],
                device_id=to, device_id_type=MESH),
            pltpu.make_async_remote_copy(
                f_send.at[s], f_recv.at[s], fs_sem.at[s], fr_sem.at[s],
                device_id=to, device_id_type=MESH),
        )

    def send_state(s):
        s_send[s] = inc_s[...].astype(BF16)
        f_send[s] = inc_f[...]

        @pl.when(me + 2 ** s < n_sp)
        def _():
            for copy in state_copies(s):
                copy.start()

    send_state(0)

    experts = n_sp * n_tp
    per_group = experts // GROUPS
    group_cap = rows_ref.shape[0] // GROUPS
    slots = per_group * capp
    id0, id1 = ids_ref[0:1, :], ids_ref[1:2, :]
    oh0 = (iota((experts, row_count), 0) == id0).astype(F32)
    oh1 = (iota((experts, row_count), 0) == id1).astype(F32)
    before = (iota((row_count, row_count), 0) < iota((row_count, row_count), 1)).astype(BF16)
    counts = dot((oh0 + oh1).astype(BF16), before)
    rank0 = jnp.sum(counts * oh0, axis=0, keepdims=True).astype(jnp.int32)
    rank1 = jnp.sum(counts * oh1, axis=0, keepdims=True).astype(jnp.int32)
    group = id0 // per_group
    ohg = (iota((16, row_count), 0) == group).astype(F32)
    rank_g = jnp.sum(dot(ohg.astype(BF16), before) * ohg, axis=0, keepdims=True).astype(jnp.int32)
    place = group * group_cap + rank_g
    gsel = (iota((GROUPS * group_cap, row_count), 0) == place).astype(F32).astype(BF16)
    gsel_ref[...] = gsel
    slot0 = (id0 - group * per_group) * capp + rank0
    slot1 = (id1 - group * per_group) * capp + rank1
    gap = logit_ref[0:1, :] - logit_ref[1:2, :]
    w0 = prob_ref[...] / (1.0 + jnp.exp(-gap))
    w1 = prob_ref[...] / (1.0 + jnp.exp(gap))
    slot_iota = iota((slots, row_count), 0)
    w_tok = jnp.where(slot_iota == slot0, w0, 0.0) + jnp.where(slot_iota == slot1, w1, 0.0)
    wc_ref[...] = dot_nt(gsel, w_tok.astype(BF16)).astype(BF16)

    for n in range(blocks):
        rows = slice(n * BLOCK, (n + 1) * BLOCK)
        for h in range(heads):
            ch = slice(h * KEY_FEATURE_DIM, (h + 1) * KEY_FEATURE_DIM)
            scores = jnp.where(tri > 0, dot_nt(qd[rows, ch], kd[rows, ch]), 0.0)
            within[rows, ch] = dot(scores.astype(BF16), v_ref[rows, ch]) + dot_nt(
                qd[rows, ch], st_in[n, h])

    for s in range(steps):
        if s > 0:
            send_state(s)

        @pl.when(me >= 2 ** s)
        def _(s=s):
            for copy in state_copies(s):
                copy.wait_recv()
            for h in range(heads):
                ch = slice(h * KEY_FEATURE_DIM, (h + 1) * KEY_FEATURE_DIM)
                got = s_recv[s, h].astype(F32)
                exc_s[h] = got * exc_f[0:1, ch] + exc_s[h]
                inc_s[h] = got * inc_f[0:1, ch] + inc_s[h]
            exc_f[...] = exc_f[...] * f_recv[s]
            inc_f[...] = inc_f[...] * f_recv[s]

    for h in range(heads):
        ch = slice(h * KEY_FEATURE_DIM, (h + 1) * KEY_FEATURE_DIM)
        out = within[:, ch] + dot_nt(rw[:, ch], exc_s[h].astype(BF16))
        mean_sq = jnp.mean(out * out, axis=-1, keepdims=True)
        out = (out * lax.rsqrt(mean_sq + EPSILON) * gain_ref[:, ch]).astype(BF16)
        for t in range(n_tp):
            attn[t, :, ch] = out[t * row_count : (t + 1) * row_count]

    def attn_copy(i):
        to = lax.rem(tp + i, n_tp)
        return pltpu.make_async_remote_copy(
            attn.at[to], arecv.at[tp], as_sem.at[i], ar_sem.at[i],
            device_id=(me, to), device_id_type=MESH)

    for i in range(1, n_tp):
        attn_copy(i).start()
    arecv[tp] = attn[tp]
    for s in range(steps):
        @pl.when(me + 2 ** s < n_sp)
        def _(s=s):
            for copy in state_copies(s):
                copy.wait_send()
    ow_copy.wait()
    for i in range(1, n_tp):
        attn_copy(i).wait_recv()
    x = jnp.concatenate([arecv[t] for t in range(n_tp)], axis=1)
    tile = 512
    total = jnp.zeros((row_count, 1), F32)
    for c in range(0, model, tile):
        cs = slice(c, c + tile)
        mixed = (stream_ref[:, cs].astype(F32) + dot(x, ow[:, cs])).astype(BF16)
        mixed_ref[:, cs] = mixed
        mixed32 = mixed.astype(F32)
        total = total + jnp.sum(mixed32 * mixed32, axis=1, keepdims=True)
    inv = lax.rsqrt(total / model + EPSILON)
    for c in range(0, model, tile):
        cs = slice(c, c + tile)
        normed = (mixed_ref[:, cs].astype(F32) * inv * ffn_ref[:, cs]).astype(BF16)
        rows_ref[:, cs] = dot(gsel_ref[...], normed).astype(BF16)
    for i in range(1, n_tp):
        attn_copy(i).wait_send()


def layer_kernel(
    n_sp, n_tp, per_group, capp,
    q_ref, k_ref, v_ref, decay_ref, gain_ref, stream_ref, ow_hbm, ffn_ref, ids_ref, prob_ref,
    logit_ref, gate_hbm, up_hbm, down_hbm,
    out_ref,
    mixed_ref, rows_ref, wc_ref, gsel_ref,
    gate, up, down, zrow, zw, stage, xbuf, hid, ybuf, back, ret, zret,
    w_sem, zs_sem, zr_sem, ws_sem, wr_sem, ps_sem, pr_sem, bs_sem, br_sem, rs_sem, rr_sem,
    *mixer_scratch,
):
    idx = lax.axis_index("sp") * n_tp + lax.axis_index("tp")
    z, p = idx // per_group, lax.rem(idx, per_group)
    cap = zrow.shape[1]
    slots = per_group * capp
    model = out_ref.shape[1]
    ff = hid.shape[1]

    def device(plane, place):
        flat = plane * per_group + place
        return (flat // n_tp, lax.rem(flat, n_tp))

    weights = [
        pltpu.make_async_copy(gate_hbm.at[0], gate, w_sem.at[0]),
        pltpu.make_async_copy(up_hbm.at[0], up, w_sem.at[1]),
        pltpu.make_async_copy(down_hbm.at[0], down, w_sem.at[2]),
    ]
    def greet():
        barrier = pltpu.get_barrier_semaphore()
        for i in range(1, GROUPS):
            pl.semaphore_signal(
                barrier, inc=1, device_id=device(lax.rem(z + i, GROUPS), p), device_id_type=MESH)

        @pl.loop(1, per_group)
        def _(i):
            pl.semaphore_signal(
                barrier, inc=1, device_id=device(z, lax.rem(p + i, per_group)),
                device_id_type=MESH)

    mixer_part(
        n_sp, n_tp, capp, greet,
        q_ref, k_ref, v_ref, decay_ref, gain_ref, stream_ref, ow_hbm, ffn_ref, ids_ref, prob_ref,
        logit_ref, mixed_ref, rows_ref, wc_ref, gsel_ref, weights, *mixer_scratch)

    def plane_rows(k):
        to = lax.rem(z + k, GROUPS)
        return (
            pltpu.make_async_remote_copy(
                wc_ref.at[pl.ds(pl.multiple_of(to * cap, cap), cap)], zw.at[k],
                ws_sem.at[k], wr_sem.at[k], device_id=device(to, p), device_id_type=MESH),
            pltpu.make_async_remote_copy(
                rows_ref.at[pl.ds(pl.multiple_of(to * cap, cap), cap)], zrow.at[k],
                zs_sem.at[k], zr_sem.at[k], device_id=device(to, p), device_id_type=MESH),
        )

    def plane_return(k):
        to = lax.rem(z + GROUPS - k, GROUPS)
        return pltpu.make_async_remote_copy(
            ret.at[k], zret.at[z], rs_sem.at[k], rr_sem.at[k],
            device_id=device(to, p), device_id_type=MESH)

    def piece(k, i):
        to = lax.rem(p + i, per_group)
        return pltpu.make_async_remote_copy(
            stage.at[k, to], xbuf.at[k, p], ps_sem.at[k, i], pr_sem.at[k, i],
            device_id=device(z, to), device_id_type=MESH)

    def piece_back(k, i):
        to = lax.rem(p + i, per_group)
        return pltpu.make_async_remote_copy(
            ybuf.at[k, to], back.at[k, p], bs_sem.at[k, i], br_sem.at[k, i],
            device_id=device(z, to), device_id_type=MESH)

    for k in range(1, GROUPS):
        for copy in plane_rows(k):
            copy.start()
    own = pl.ds(pl.multiple_of(z * cap, cap), cap)
    zrow[0] = rows_ref[own, :]
    zw[0] = wc_ref[own, :]
    tile = 512

    def dispatch(k):
        if k > 0:
            for copy in plane_rows(k):
                copy.wait_recv()
        sel = (zw[k].astype(F32) > 0).astype(F32).astype(BF16)
        for c in range(0, model, tile):
            cs = slice(c, c + tile)
            stage[k, :, :, cs] = dot_tn(sel, zrow[k, :, cs]).astype(BF16).reshape(
                per_group, capp, tile)

        @pl.loop(1, per_group)
        def _(i):
            piece(k, i).start()

        xbuf[k, p] = stage[k, p]

    def expert(k):
        @pl.loop(1, per_group)
        def _(i):
            piece(k, i).wait_recv()

        x = xbuf.at[k]

        @pl.loop(0, ff // 256)
        def _(f):
            fs = pl.ds(pl.multiple_of(f * 256, 256), 256)
            rows = x[...].reshape(slots, model)
            g = dot(rows, gate[:, fs])
            u = dot(rows, up[:, fs])
            hid[:, fs] = (g / (1.0 + jnp.exp(-g)) * u).astype(BF16)

        @pl.loop(0, model // tile)
        def _(c):
            cs = pl.ds(pl.multiple_of(c * tile, tile), tile)
            ybuf[k, :, :, cs] = dot(hid[...], down[:, cs]).astype(BF16).reshape(
                per_group, capp, tile)

        @pl.loop(1, per_group)
        def _(i):
            piece_back(k, i).start()

        back[k, p] = ybuf[k, p]

    def combine(k):
        @pl.loop(1, per_group)
        def _(i):
            piece_back(k, i).wait_recv()

        w = zw[k]
        for c in range(0, model, tile):
            cs = slice(c, c + tile)
            y = dot(w, back[k, :, :, cs].reshape(slots, tile)).astype(BF16)
            if k == 0:
                zret[z, :, cs] = y
            else:
                ret[k, :, cs] = y
        if k > 0:
            plane_return(k).start()

    for step in SCHEDULE.split():
        if step == "W":
            for copy in weights:
                copy.wait()
        else:
            {"D": dispatch, "E": expert, "C": combine}[step[0]](int(step[1]))

    for k in range(1, GROUPS):
        plane_return(k).wait_recv()
    for c in range(0, model, tile):
        cs = slice(c, c + tile)
        moved = dot_tn(gsel_ref[...], zret[:, :, cs].reshape(GROUPS * cap, tile))
        out_ref[:, cs] = (mixed_ref[:, cs].astype(F32) + moved).astype(BF16)

    for k in range(1, GROUPS):
        for copy in plane_rows(k):
            copy.wait_send()
        plane_return(k).wait_send()
    for k in range(GROUPS):
        @pl.loop(1, per_group)
        def _(i, k=k):
            piece(k, i).wait_send()
            piece_back(k, i).wait_send()


def local(
    stream, query_rows, key_rows, value_rows, log_decay, head_gain, out_weight, ffn_gain,
    expert_ids, group_prob, pick_logits, gate_weight, up_weight, down_weight,
):
    n_sp, n_tp = lax.axis_size("sp"), lax.axis_size("tp")
    tokens, cols = query_rows.shape
    heads = cols // KEY_FEATURE_DIM
    blocks = tokens // BLOCK
    row_count, model = stream.shape
    devices = n_sp * n_tp
    per_group = devices // GROUPS
    cap = 2 * row_count * TOPK // devices
    capp = -(-cap // 16) * 16
    group_cap = per_group * cap // TOPK
    slots = per_group * capp
    ff = gate_weight.shape[2]
    steps = max(1, (n_sp - 1).bit_length())
    kd = KEY_FEATURE_DIM
    vm = pl.BlockSpec(memory_space=pltpu.VMEM)
    anyspace = pl.BlockSpec(memory_space=pl.ANY)
    dma = pltpu.SemaphoreType.DMA
    mixer_scratch = [
        pltpu.VMEM((tokens, cols), BF16),
        pltpu.VMEM((tokens, cols), BF16),
        pltpu.VMEM((tokens, cols), BF16),
        pltpu.VMEM((blocks, heads, kd, kd), BF16),
        pltpu.VMEM((tokens, cols), F32),
        pltpu.VMEM(out_weight.shape, BF16),
        pltpu.VMEM((heads, kd, kd), F32),
        pltpu.VMEM((8, cols), F32),
        pltpu.VMEM((heads, kd, kd), F32),
        pltpu.VMEM((8, cols), F32),
        pltpu.VMEM((steps, heads, kd, kd), BF16),
        pltpu.VMEM((steps, heads, kd, kd), BF16),
        pltpu.VMEM((steps, 8, cols), F32),
        pltpu.VMEM((steps, 8, cols), F32),
        pltpu.VMEM((n_tp, row_count, cols), BF16),
        pltpu.VMEM((n_tp, row_count, cols), BF16),
        dma,
        dma((steps,)), dma((steps,)), dma((steps,)), dma((steps,)),
        dma((n_tp,)), dma((n_tp,)),
    ]
    return pl.pallas_call(
        functools.partial(layer_kernel, n_sp, n_tp, per_group, capp),
        out_shape=jax.ShapeDtypeStruct((row_count, model), BF16),
        in_specs=[vm] * 6 + [anyspace] + [vm] * 4 + [anyspace] * 3,
        out_specs=vm,
        scratch_shapes=[
            pltpu.VMEM((row_count, model), BF16),
            pltpu.VMEM((GROUPS * group_cap, model), BF16),
            pltpu.VMEM((GROUPS * group_cap, slots), BF16),
            pltpu.VMEM((GROUPS * group_cap, row_count), BF16),
            pltpu.VMEM((model, ff), BF16),
            pltpu.VMEM((model, ff), BF16),
            pltpu.VMEM((ff, model), BF16),
            pltpu.VMEM((GROUPS, group_cap, model), BF16),
            pltpu.VMEM((GROUPS, group_cap, slots), BF16),
            pltpu.VMEM((GROUPS, per_group, capp, model), BF16),
            pltpu.VMEM((GROUPS, per_group, capp, model), BF16),
            pltpu.VMEM((slots, ff), BF16),
            pltpu.VMEM((GROUPS, per_group, capp, model), BF16),
            pltpu.VMEM((GROUPS, per_group, capp, model), BF16),
            pltpu.VMEM((GROUPS, group_cap, model), BF16),
            pltpu.VMEM((GROUPS, group_cap, model), BF16),
            dma((3,)),
            dma((GROUPS,)), dma((GROUPS,)), dma((GROUPS,)), dma((GROUPS,)),
            dma((GROUPS, per_group)), dma((GROUPS, per_group)),
            dma((GROUPS, per_group)), dma((GROUPS, per_group)),
            dma((GROUPS,)), dma((GROUPS,)),
        ] + mixer_scratch,
        compiler_params=pltpu.CompilerParams(
            collective_id=0, has_side_effects=True, vmem_limit_bytes=VMEM_LIMIT),
    )(
        query_rows, key_rows, value_rows, log_decay, head_gain[None], stream, out_weight,
        ffn_gain[None], expert_ids.T, group_prob[None], pick_logits.T,
        gate_weight, up_weight, down_weight,
    )


def solution(mesh):
    in_specs = (
        P(("sp", "tp"), None),
        P("sp", "tp"),
        P("sp", "tp"),
        P("sp", "tp"),
        P("sp", "tp"),
        P("tp"),
        P(),
        P(),
        P(("sp", "tp"), None),
        P(("sp", "tp")),
        P(("sp", "tp"), None),
        P(("sp", "tp"), None, None),
        P(("sp", "tp"), None, None),
        P(("sp", "tp"), None, None),
    )
    out_specs = P(("sp", "tp"), None)
    return jax.shard_map(local, mesh=mesh, in_specs=in_specs, out_specs=out_specs, check_vma=False)
```
